32 devices in a mesh: ep: 8 (over z, y), tp: 4 (over x, core).
Axes of the slice: x: 2, y: 2, z: 4, core: 2. Of those that a mesh axis runs over, the one named last changes fastest.
Arguments:
- tokens: bfloat16 [256, 2048], P('ep'), may hold values from -6 to 6
- gain_mix: bfloat16 [2048], replicated, may hold values from 0.099609375 to 1.8984375
- gain_ffn: bfloat16 [2048], replicated, may hold values from 0.099609375 to 1.8984375
- w_query: bfloat16 [2048, 1024], P('ep', 'tp'), may hold values from -0.125 to 0.125
- w_key: bfloat16 [2048, 1024], P('ep', 'tp'), may hold values from -0.125 to 0.125
- w_value: bfloat16 [2048, 1024], P('ep', 'tp'), may hold values from -0.125 to 0.125
- w_outgate: bfloat16 [2048, 1024], P('ep', 'tp'), may hold values from -0.125 to 0.125
- w_ingate: bfloat16 [2048, 8], replicated, may hold values from -0.125 to 0.125
- w_forget: bfloat16 [2048, 8], replicated, may hold values from -0.125 to 0.125
- bias_in: float32 [8], replicated, may hold values from -2 to 2
- bias_forget: float32 [8], replicated, may hold values from -1 to 3
- w_proj: bfloat16 [1024, 2048], P('tp'), may hold values from -0.1875 to 0.1875
- matrix_state: float32 [256, 8, 128, 128], P('ep', 'tp'), may hold values from -0.6 to 0.6
- normal_state: float32 [256, 8, 128], P('ep', 'tp'), may hold values from -0.6 to 0.6
- stab_state: float32 [256, 8], P('ep', 'tp'), may hold values from -1 to 1
- route_ids: int32 [256, 2], P('ep'), may hold values from 0 to 3, all different within a row; in each aligned block of 32 rows (0 to 31, 32 to 63, ...) at most 32 rows name the same one
- route_weights: float32 [256, 2], P('ep'), may hold values from 0.1 to 1
- w_exp_gate: bfloat16 [8, 2048, 1536], P('ep', None, 'tp'), may hold values from -0.125 to 0.125
- w_exp_up: bfloat16 [8, 2048, 1536], P('ep', None, 'tp'), may hold values from -0.125 to 0.125
- w_exp_down: bfloat16 [8, 1536, 2048], P('ep', 'tp'), may hold values from -0.109375 to 0.109375
Outputs:
- mixed_out: bfloat16 [256, 2048], P('ep', 'tp')
- matrix_out: float32 [256, 8, 128, 128], P('ep', 'tp')
- normal_out: float32 [256, 8, 128], P('ep', 'tp')
- stab_out: float32 [256, 8], P('ep', 'tp')
The draws below stay inside these ranges and needn't reach their ends.
Inputs may be any that keep to these rules, and one draw needn't show every extreme that they name: `route_ids`: each row names 2 different experts; among the rows of one index of ep no expert is named by more than 32 rows, and in every draw some expert is named by exactly 32 of them.
All inputs are finite; a program needn't handle non-finite values.
Results may differ from the reference program's by a relative error of at most 0.015.
Values may be sent and summed in bfloat16 or wider, within the bound.
A program may use at most 64 MiB of HBM per device.

```python
import math
import jax
import jax.numpy as jnp
import numpy as np
from jax import lax

D = 2048
HEADS = 8
HEAD_DIM = 128
FF = 3072
TOPK = 2
SEQ_DEV = 32
WIDTH = 1024
SEQS = 256
EXPERTS = 4
CAP = 32
N_EP = 8
N_TP = 4


def shard_levels(stream_key, extent, split, low, largest):
    level = 1.0
    for dim, shards_of in split:
        draws = jax.random.uniform(jax.random.fold_in(jax.random.fold_in(stream_key, 6), dim), (shards_of,), jnp.float32, low / len(split), largest / len(split))
        level = level * jnp.repeat(jnp.exp(draws), extent[dim] // shards_of).reshape((-1,) + (1,) * (len(extent) - 1 - dim))
    return level


def shared_out(own_key, own, number, rows, count, top, most, lean):
    order = jax.random.permutation(own_key, count)
    heavy_load, common = portions_of(count, rows * top, most, lean, True), portions_of(count, rows * top, most, lean, False)
    places = jnp.arange(count)

    def named(tallies, turn):
        used = int((tallies > 0).sum())
        fixed = max(1, used // 4)
        moved = fixed + (places - fixed + turn * (used - fixed)) % max(1, count - fixed)
        return jnp.zeros((count,), jnp.int32).at[order[jnp.where(places < fixed, places, moved)]].set(jnp.asarray(tallies, jnp.int32))

    tallies = jnp.where(number % 4 == 0, named(heavy_load, number // 4), named(common, number - number // 4 - 1))
    mixed = jax.random.permutation(jax.random.fold_in(own, 3), count)
    donor, sink = mixed[0:count // 2 * 2:2], mixed[1:count // 2 * 2:2]
    room = jnp.minimum(tallies[donor] - 1, most - tallies[sink]) // 2
    room = jnp.where((donor == order[0]) | (sink == order[0]) | (tallies[sink] == 0), 0, jnp.maximum(room, 0))
    moved = jax.random.randint(jax.random.fold_in(own, 4), (count // 2,), 0, 1 << 20) % (room + 1)
    tallies = tallies.at[donor].add(-moved).at[sink].add(moved)
    items = jnp.searchsorted(jnp.cumsum(tallies), jnp.arange(rows * top), side="right").astype(jnp.int32)
    table = items.reshape(top, rows).T
    table = table[jax.random.permutation(jax.random.fold_in(own, 1), rows)]
    turn = jax.random.randint(jax.random.fold_in(own, 2), (rows, 1), 0, top)
    return jnp.take_along_axis(table, (jnp.arange(top)[None, :] + turn) % top, axis=1)


def portions_of(number_of, total, most, lean, full):
    portions = [(1 << 20) // math.isqrt(grade ** lean) + 1 for grade in range(1, number_of + 1)]
    largest = most if full else min(most, max(-(-total // number_of), total * portions[0] // sum(portions)))
    least = 1 if total - largest >= number_of - 1 else 0
    holding, surplus = [largest] + [least] * (number_of - 1), total - largest - least * (number_of - 1)
    while surplus > 0:
        movable = [i for i in range(1, number_of) if holding[i] < largest] or [i for i in range(1, number_of) if holding[i] < most]
        mass, budget = sum([portions[i] for i in movable]), surplus
        for i in movable:
            extra = min(most - holding[i], max(1, budget * portions[i] // mass), surplus)
            holding[i] = holding[i] + extra
            surplus = surplus - extra
    return np.array(holding)


def scatter_about(stream_key, dims, width, reach, split=(), held_as=jnp.bfloat16):
    level = shard_levels(stream_key, dims, split, -0.22, 0.18) if split else 1.0
    values = jax.random.normal(stream_key, dims, jnp.float32) * width * level
    return jnp.minimum(jnp.maximum(values, -reach), reach).astype(held_as)


def setup_inputs(seed: int = 0) -> dict:
    splits = jax.random.split(jax.random.key(seed), 21)
    tokens = scatter_about(splits[0], (SEQS, D), 1.0, 6.0, ((0, 8),))
    gain_mix = jnp.clip(1.0 + 0.18 * jax.random.normal(splits[1], (D,), jnp.float32), 0.099609375, 1.8984375).astype(jnp.bfloat16)
    gain_ffn = jnp.clip(1.0 + 0.18 * jax.random.normal(splits[2], (D,), jnp.float32), 0.099609375, 1.8984375).astype(jnp.bfloat16)
    w_query = scatter_about(splits[3], (D, WIDTH), D ** -0.5, 0.125, ((0, 8), (1, 4)))
    w_key = scatter_about(splits[4], (D, WIDTH), D ** -0.5, 0.125, ((0, 8), (1, 4)))
    w_value = scatter_about(splits[5], (D, WIDTH), D ** -0.5, 0.125, ((0, 8), (1, 4)))
    w_outgate = scatter_about(splits[6], (D, WIDTH), D ** -0.5, 0.125, ((0, 8), (1, 4)))
    w_ingate = scatter_about(splits[7], (D, HEADS), D ** -0.5, 0.125)
    w_forget = scatter_about(splits[8], (D, HEADS), D ** -0.5, 0.125)
    bias_in = jnp.clip(jax.random.uniform(splits[9], (HEADS,), jnp.float32, -2.0, 2.0), -2.0, 2.0)
    bias_forget = jnp.clip(jax.random.uniform(splits[10], (HEADS,), jnp.float32, -1.0, 3.0), -1.0, 3.0)
    w_proj = scatter_about(splits[11], (WIDTH, D), WIDTH ** -0.5, 0.1875, ((0, 4),))
    matrix_state = scatter_about(splits[12], (SEQS, HEADS, HEAD_DIM, HEAD_DIM), 0.1, 0.6, ((0, 8), (1, 4)), jnp.float32)
    normal_state = scatter_about(splits[13], (SEQS, HEADS, HEAD_DIM), 0.1, 0.6, ((0, 8), (1, 4)), jnp.float32)
    stab_state = jnp.clip(jax.random.uniform(splits[14], (SEQS, HEADS), jnp.float32, -1.0, 1.0) * shard_levels(splits[14], (SEQS, HEADS), ((0, 8), (1, 4)), -0.4, 0.0), -1.0, 1.0)
    route_ids_keys = jax.random.split(jax.random.fold_in(splits[15], 1), SEQS // SEQ_DEV)
    route_ids_turns = jax.random.permutation(jax.random.fold_in(splits[15], 3), SEQS // SEQ_DEV)
    route_ids = jax.vmap(lambda own, number: shared_out(jax.random.fold_in(splits[15], 2), own, number, SEQ_DEV, EXPERTS, TOPK, CAP, 1))(route_ids_keys, route_ids_turns).reshape((SEQS, TOPK))
    route_weights = jnp.clip(0.1 + 0.9 * jax.random.uniform(splits[16], (SEQS, TOPK), jnp.float32) ** shard_levels(splits[16], (SEQS, TOPK), ((0, 8),), -0.2, 0.2), 0.1, 1.0)
    w_exp_gate = scatter_about(splits[17], (2 * EXPERTS, D, FF // 2), D ** -0.5, 0.125, ((0, 8), (2, 4)))
    w_exp_up = scatter_about(splits[18], (2 * EXPERTS, D, FF // 2), D ** -0.5, 0.125, ((0, 8), (2, 4)))
    w_exp_down = scatter_about(splits[19], (2 * EXPERTS, FF // 2, D), FF ** -0.5, 0.109375, ((0, 8), (1, 4)))
    return {"tokens": tokens, "gain_mix": gain_mix, "gain_ffn": gain_ffn, "w_query": w_query, "w_key": w_key, "w_value": w_value, "w_outgate": w_outgate, "w_ingate": w_ingate, "w_forget": w_forget, "bias_in": bias_in, "bias_forget": bias_forget, "w_proj": w_proj, "matrix_state": matrix_state, "normal_state": normal_state, "stab_state": stab_state, "route_ids": route_ids, "route_weights": route_weights, "w_exp_gate": w_exp_gate, "w_exp_up": w_exp_up, "w_exp_down": w_exp_down}


norm_epsilon = 1e-06

def rms_scale(row_block, gain):
    wide = row_block.astype(jnp.float32)
    factor = lax.rsqrt(lax.optimization_barrier(jnp.mean(wide * wide, axis=-1, keepdims=True)) + norm_epsilon)
    return (wide * factor * gain.astype(jnp.float32)).astype(jnp.bfloat16)

def memory_step(query, key_rows, value_rows, gate_rows, in_pre, forget_pre, matrix_state, normal_state, stab_state):
    log_forget = jax.nn.log_sigmoid(forget_pre)
    stab_new = jnp.maximum(log_forget + stab_state, in_pre)
    carry = jnp.exp(log_forget + stab_state - stab_new)
    inflow = jnp.exp(in_pre - stab_new)
    scaled_keys = key_rows.astype(jnp.float32) * query.shape[-1] ** (-0.5)
    value_wide = value_rows.astype(jnp.float32)
    matrix_new = carry[..., None, None] * matrix_state + inflow[..., None, None] * scaled_keys[..., :, None] * value_wide[..., None, :]
    normal_new = carry[..., None] * normal_state + inflow[..., None] * scaled_keys
    query_wide = query.astype(jnp.float32)
    numer = jnp.einsum('shd,shde->she', query_wide, matrix_new, precision=lax.Precision.HIGHEST)
    denom = jnp.maximum(jnp.abs(lax.optimization_barrier(jnp.sum(query_wide * normal_new, axis=-1))), 1.0)
    hidden = numer / denom[..., None] * jax.nn.sigmoid(gate_rows.astype(jnp.float32))
    return (hidden, matrix_new, normal_new, stab_new)

def reference(tokens, gain_mix, gain_ffn, w_query, w_key, w_value, w_outgate, w_ingate, w_forget, bias_in, bias_forget, w_proj, matrix_state, normal_state, stab_state, route_ids, route_weights, w_exp_gate, w_exp_up, w_exp_down):
    normed = rms_scale(tokens, gain_mix)

    def project(weight):
        return jnp.dot(normed, weight, preferred_element_type=jnp.float32).astype(jnp.bfloat16).reshape(SEQS, HEADS, HEAD_DIM)
    query = project(w_query)
    key_rows = project(w_key)
    value_rows = project(w_value)
    gate_rows = project(w_outgate)
    in_pre = jnp.dot(normed, w_ingate, preferred_element_type=jnp.float32) + bias_in
    forget_pre = jnp.dot(normed, w_forget, preferred_element_type=jnp.float32) + bias_forget
    hidden, matrix_new, normal_new, stab_new = memory_step(query, key_rows, value_rows, gate_rows, in_pre, forget_pre, matrix_state, normal_state, stab_state)
    cell = hidden.reshape(SEQS, WIDTH).astype(jnp.bfloat16)
    group_terms = jnp.einsum('sbw,bwd->bsd', cell.reshape(SEQS, N_TP, WIDTH // N_TP).astype(jnp.float32), w_proj.reshape(N_TP, WIDTH // N_TP, D).astype(jnp.float32))
    group_terms = lax.optimization_barrier(group_terms.astype(jnp.bfloat16))
    attended = lax.optimization_barrier(jnp.sum(group_terms.astype(jnp.float32), axis=0))
    resid = (tokens.astype(jnp.float32) + attended).astype(jnp.bfloat16)
    normed_ffn = rms_scale(resid, gain_ffn)
    flat_ids = route_ids.reshape(N_EP, SEQ_DEV * TOPK).astype(jnp.int32)
    expert_hot = (flat_ids[..., None] == jnp.arange(EXPERTS, dtype=jnp.int32)).astype(jnp.int32)
    slot_rank = lax.optimization_barrier(jnp.sum((jnp.cumsum(expert_hot, axis=1).astype(jnp.int32) - 1) * expert_hot, axis=-1)).astype(jnp.int32)
    placed = (jnp.arange(N_EP, dtype=jnp.int32)[:, None] * CAP + slot_rank).astype(jnp.int32)
    routed_rows = jnp.repeat(normed_ffn, TOPK, axis=0).reshape(N_EP, SEQ_DEV * TOPK, D)
    buffer = jnp.zeros((EXPERTS, N_EP * CAP, D), jnp.bfloat16).at[flat_ids, placed].set(routed_rows)
    quarter = FF // (2 * N_TP)

    def expert(operands):
        inputs, gate_pair, up_pair, down_pair = operands
        results = []
        for half_index in range(2):
            gate_sum = jnp.dot(inputs, gate_pair[half_index], preferred_element_type=jnp.float32)
            up_sum = jnp.dot(inputs, up_pair[half_index], preferred_element_type=jnp.float32)
            inner = (jax.nn.silu(gate_sum) * up_sum).astype(jnp.bfloat16)
            quarters = jnp.einsum('rtf,tfd->trd', inner.reshape(N_EP * CAP, N_TP, quarter).astype(jnp.float32), down_pair[half_index].reshape(N_TP, quarter, D).astype(jnp.float32))
            quarters = lax.optimization_barrier(quarters.astype(jnp.bfloat16))
            results.append(lax.optimization_barrier(jnp.sum(quarters.astype(jnp.float32), axis=0)).astype(jnp.bfloat16))
        return jnp.stack(results)
    outputs = lax.map(expert, (buffer, w_exp_gate.reshape(EXPERTS, 2, D, FF // 2), w_exp_up.reshape(EXPERTS, 2, D, FF // 2), w_exp_down.reshape(EXPERTS, 2, FF // 2, D)))
    picked = outputs[flat_ids, :, placed]
    both_halves = lax.optimization_barrier(jnp.sum(picked.astype(jnp.float32), axis=2)).reshape(SEQS, TOPK, D)
    weights = route_weights / lax.optimization_barrier(jnp.sum(route_weights, axis=-1, keepdims=True))
    routed = lax.optimization_barrier(jnp.sum(weights[..., None] * both_halves, axis=1))
    mixed_out = (resid.astype(jnp.float32) + routed).astype(jnp.bfloat16)
    return (mixed_out, matrix_new, normal_new, stab_new)
```

```python
import functools

import jax
import jax.numpy as jnp
from jax import lax
from jax.experimental import pallas as pl
from jax.experimental.pallas import tpu as pltpu
from jax.sharding import PartitionSpec as P

norm_epsilon = 1e-06
MESH = pl.DeviceIdType.MESH


def rms_scale(row_block, gain):
    wide = row_block.astype(jnp.float32)
    factor = lax.rsqrt(jnp.mean(wide * wide, axis=-1, keepdims=True) + norm_epsilon)
    return (wide * factor * gain.astype(jnp.float32)).astype(jnp.bfloat16)


def memory_step(
    query,
    key_rows,
    value_rows,
    gate_rows,
    in_pre,
    forget_pre,
    matrix_state,
    normal_state,
    stab_state,
):
    log_forget = jax.nn.log_sigmoid(forget_pre)
    stab_new = jnp.maximum(log_forget + stab_state, in_pre)
    carry = jnp.exp(log_forget + stab_state - stab_new)
    inflow = jnp.exp(in_pre - stab_new)
    scaled_keys = key_rows.astype(jnp.float32) * query.shape[-1] ** (-0.5)
    value_wide = value_rows.astype(jnp.float32)
    matrix_new = (
        carry[..., None, None] * matrix_state
        + inflow[..., None, None] * scaled_keys[..., :, None] * value_wide[..., None, :]
    )
    normal_new = carry[..., None] * normal_state + inflow[..., None] * scaled_keys
    query_wide = query.astype(jnp.float32)
    numer = jnp.einsum("shd,shde->she", query_wide, matrix_new, precision=lax.Precision.HIGHEST)
    denom = jnp.maximum(jnp.abs(jnp.sum(query_wide * normal_new, axis=-1)), 1.0)
    hidden = numer / denom[..., None] * jax.nn.sigmoid(gate_rows.astype(jnp.float32))
    return (hidden, matrix_new, normal_new, stab_new)


def gather_project_kernel(ep_count, tokens_ref, gain_ref, wq_ref, wk_ref, wv_ref, wo_ref, out_ref,
                          blocks, foreign, terms, landed, s1, r1, s2, r2):
    me = lax.axis_index("ep")

    def peer(step):
        return lax.rem(me + step, ep_count)

    def source(step):
        return lax.rem(me - step + ep_count, ep_count)

    barrier = pltpu.get_barrier_semaphore()

    @pl.loop(1, ep_count)
    def _(step):
        pl.semaphore_signal(barrier, inc=1, device_id={"ep": peer(step)}, device_id_type=MESH)

    depth = wq_ref.shape[0]
    wide = tokens_ref[...].astype(jnp.float32)
    factor = lax.rsqrt(jnp.mean(wide * wide, axis=-1, keepdims=True) + norm_epsilon)
    normed = (wide * factor * gain_ref[...].astype(jnp.float32)).astype(jnp.bfloat16)
    for part in range(ep_count):
        blocks[part] = normed[:, part * depth : (part + 1) * depth]
    pl.semaphore_wait(barrier, ep_count - 1)

    def first(step):
        return pltpu.make_async_remote_copy(
            src_ref=blocks.at[peer(step)], dst_ref=foreign.at[me],
            send_sem=s1.at[step], recv_sem=r1.at[step],
            device_id={"ep": peer(step)}, device_id_type=MESH)

    def first_landing(step):
        return pltpu.make_async_remote_copy(
            src_ref=blocks.at[peer(step)], dst_ref=foreign.at[source(step)],
            send_sem=s1.at[step], recv_sem=r1.at[step],
            device_id={"ep": peer(step)}, device_id_type=MESH)

    def second(index, step):
        return pltpu.make_async_remote_copy(
            src_ref=terms.at[index, peer(step)], dst_ref=landed.at[index, me],
            send_sem=s2.at[index, step], recv_sem=r2.at[index, step],
            device_id={"ep": peer(step)}, device_id_type=MESH)

    def second_landing(index, step):
        return pltpu.make_async_remote_copy(
            src_ref=terms.at[index, peer(step)], dst_ref=landed.at[index, source(step)],
            send_sem=s2.at[index, step], recv_sem=r2.at[index, step],
            device_id={"ep": peer(step)}, device_id_type=MESH)

    @pl.loop(1, ep_count)
    def _(step):
        first(step).start()

    foreign[me] = blocks[me]

    @pl.loop(1, ep_count)
    def _(step):
        first_landing(step).wait_recv()

    rows = tokens_ref.shape[0]
    all_rows = foreign[...].reshape(ep_count * rows, depth)
    for index, weight in enumerate((wq_ref, wk_ref, wv_ref, wo_ref)):
        product = jnp.dot(all_rows, weight[...], preferred_element_type=jnp.float32)
        terms[index] = product.astype(jnp.bfloat16).reshape(ep_count, rows, weight.shape[1])

        @pl.loop(1, ep_count)
        def _(step):
            second(index, step).start()

        landed[index, me] = terms[index, me]

    for index in range(4):
        @pl.loop(1, ep_count)
        def _(step):
            second_landing(index, step).wait_recv()

        out_ref[index] = jnp.sum(landed[index].astype(jnp.float32), axis=0).astype(jnp.bfloat16)

    @pl.loop(1, ep_count)
    def _(step):
        first(step).wait_send()
        for index in range(4):
            second(index, step).wait_send()


def gather_project(tokens, gain, weights):
    ep_count = lax.axis_size("ep")
    rows = tokens.shape[0]
    depth, cols = weights[0].shape
    vmem = pl.BlockSpec(memory_space=pltpu.VMEM)
    return pl.pallas_call(
        functools.partial(gather_project_kernel, ep_count),
        out_shape=jax.ShapeDtypeStruct((4, rows, cols), jnp.bfloat16),
        in_specs=[vmem] * 6,
        out_specs=vmem,
        scratch_shapes=[
            pltpu.VMEM((ep_count, rows, depth), jnp.bfloat16),
            pltpu.VMEM((ep_count, rows, depth), jnp.bfloat16),
            pltpu.VMEM((4, ep_count, rows, cols), jnp.bfloat16),
            pltpu.VMEM((4, ep_count, rows, cols), jnp.bfloat16),
            pltpu.SemaphoreType.DMA((ep_count,)),
            pltpu.SemaphoreType.DMA((ep_count,)),
            pltpu.SemaphoreType.DMA((4, ep_count)),
            pltpu.SemaphoreType.DMA((4, ep_count)),
        ],
        compiler_params=pltpu.CompilerParams(
            collective_id=0, has_side_effects=True, vmem_limit_bytes=40 << 20),
        name="gather_project",
    )(tokens, gain.reshape(1, -1), *weights)


def experts_kernel(ep_count, tp_count, cell_ref, tokens_ref, gain_ref, table_ref, wproj_ref,
                   gate_hbm, up_hbm, down_hbm, out_ref,
                   gate_w, up_w, down_w, attn, attn_in, held, normed, inner, tables,
                   scaled, pair_in, half, half_in, share, share_in,
                   w_sem, as_, ar_, ts_, tr_, cs_, cr_, xs_, xr_, ys_, yr_, zs_, zr_,
                   ps_, pr_, us_, ur_, vs_, vr_):
    e = lax.axis_index("ep")
    t = lax.axis_index("tp")
    rows = tokens_ref.shape[0]
    cw = out_ref.shape[1]
    total = ep_count * rows
    near = t + 1 - 2 * lax.rem(t, 2)
    far = lax.rem(t + 2, tp_count)
    across = near + 2 - 4 * (near // 2)

    def peer(step):
        return lax.rem(e + step, ep_count)

    def source(step):
        return lax.rem(e - step + ep_count, ep_count)

    def remote(src, dst, ssem, rsem, target):
        return pltpu.make_async_remote_copy(
            src_ref=src, dst_ref=dst, send_sem=ssem, recv_sem=rsem,
            device_id=target, device_id_type=MESH)

    barrier = pltpu.get_barrier_semaphore()

    @pl.loop(1, ep_count)
    def _(step):
        pl.semaphore_signal(barrier, inc=1, device_id={"ep": peer(step)}, device_id_type=MESH)

    for step in range(1, tp_count):
        pl.semaphore_signal(barrier, inc=1, device_id={"tp": lax.rem(t + step, tp_count)},
                            device_id_type=MESH)
    loads = [pltpu.make_async_copy(src.at[0], dst, w_sem.at[i]) for i, (src, dst) in enumerate(
        ((gate_hbm, gate_w), (up_hbm, up_w), (down_hbm, down_w)))]
    for load in loads:
        load.start()
    cell = cell_ref[...]
    for quarter in range(tp_count):
        attn[quarter] = jnp.dot(
            cell, wproj_ref[:, quarter * cw : (quarter + 1) * cw],
            preferred_element_type=jnp.float32).astype(jnp.bfloat16)
    pl.semaphore_wait(barrier, ep_count - 1 + tp_count - 1)

    def attn_out(step):
        to = lax.rem(t + step, tp_count)
        return remote(attn.at[to], attn_in.at[t], as_.at[step], ar_.at[step], {"tp": to})

    def attn_land(step):
        to = lax.rem(t + step, tp_count)
        frm = lax.rem(t - step + tp_count, tp_count)
        return remote(attn.at[to], attn_in.at[frm], as_.at[step], ar_.at[step], {"tp": to})

    for step in range(1, tp_count):
        attn_out(step).start()
    attn_in[t] = attn[t]

    def table_out(step):
        return remote(table_ref, tables.at[e], ts_.at[step], tr_.at[step], {"ep": peer(step)})

    def table_land(step):
        return remote(table_ref, tables.at[source(step)], ts_.at[step], tr_.at[step],
                      {"ep": peer(step)})

    for step in range(1, tp_count):
        attn_land(step).wait_recv()
    attended = jnp.sum(attn_in[...].astype(jnp.float32), axis=0)
    own_tokens = tokens_ref[:, pl.ds(pl.multiple_of(t * cw, cw), cw)].astype(jnp.float32)
    held[e, t] = (own_tokens + attended).astype(jnp.bfloat16)

    def row_out(step):
        return remote(held.at[e, t], held.at[e, t], cs_.at[step], cr_.at[step],
                      {"ep": peer(step)})

    def row_land(step):
        return remote(held.at[e, t], held.at[source(step), t], cs_.at[step], cr_.at[step],
                      {"ep": peer(step)})

    def far_out(step):
        s = source(step)
        return remote(held.at[s, t], held.at[s, t], xs_.at[step], xr_.at[step], {"tp": far})

    def far_land(step):
        s = source(step)
        return remote(held.at[s, t], held.at[s, far], xs_.at[step], xr_.at[step], {"tp": far})

    def near_out(step):
        s = source(step)
        return remote(held.at[s, t], held.at[s, t], ys_.at[step], yr_.at[step], {"tp": near})

    def near_land(step):
        s = source(step)
        return remote(held.at[s, t], held.at[s, near], ys_.at[step], yr_.at[step], {"tp": near})

    def relay_out(step):
        s = source(step)
        return remote(held.at[s, far], held.at[s, far], zs_.at[step], zr_.at[step], {"tp": near})

    def relay_land(step):
        s = source(step)
        return remote(held.at[s, far], held.at[s, across], zs_.at[step], zr_.at[step],
                      {"tp": near})

    @pl.loop(1, ep_count)
    def _(step):
        row_out(step).start()

    far_out(0).start()
    near_out(0).start()

    @pl.loop(1, ep_count)
    def _(step):
        table_out(step).start()

    tables[e] = table_ref[...]

    @pl.loop(1, ep_count)
    def _(step):
        row_land(step).wait_recv()
        far_out(step).start()
        near_out(step).start()

    @pl.loop(0, ep_count)
    def _(step):
        far_land(step).wait_recv()
        relay_out(step).start()

    @pl.loop(0, ep_count)
    def _(step):
        near_land(step).wait_recv()
        relay_land(step).wait_recv()
        s = source(step)
        parts = [held[s, quarter].astype(jnp.float32) for quarter in range(tp_count)]
        square = sum(jnp.sum(part * part, axis=-1, keepdims=True) for part in parts)
        factor = lax.rsqrt(square / (cw * tp_count) + norm_epsilon)
        for quarter in range(tp_count):
            gain = gain_ref[:, quarter * cw : (quarter + 1) * cw].astype(jnp.float32)
            normed[pl.ds(pl.multiple_of(s * rows, rows), rows), quarter * cw : (quarter + 1) * cw] = (
                parts[quarter] * factor * gain).astype(jnp.bfloat16)

    @pl.loop(1, ep_count)
    def _(step):
        table_land(step).wait_recv()

    loads[0].wait()
    loads[1].wait()
    owners = min(8, ep_count)
    chunk = owners * rows
    chunks = total // chunk

    @pl.loop(0, chunks)
    def _(index):
        window = pl.ds(pl.multiple_of(index * chunk, chunk), chunk)
        block = normed[window, :]
        gate_sum = jnp.dot(block, gate_w[...], preferred_element_type=jnp.float32)
        up_sum = jnp.dot(block, up_w[...], preferred_element_type=jnp.float32)
        inner[window, :] = (gate_sum * jax.nn.sigmoid(gate_sum) * up_sum).astype(jnp.bfloat16)

    loads[2].wait()

    def down(quarter):
        @pl.loop(0, chunks)
        def _(index):
            window = pl.ds(pl.multiple_of(index * chunk, chunk), chunk)
            group = pl.ds(index * owners, owners)
            product = jnp.dot(
                inner[window, :], down_w[:, pl.ds(pl.multiple_of(quarter * cw, cw), cw)],
                preferred_element_type=jnp.float32)
            lanes = lax.broadcasted_iota(jnp.int32, (owners, rows, table_ref.shape[1]), 2)
            weight = jnp.sum(jnp.where(lanes == e // 2, tables[group], 0.0), axis=-1, keepdims=True)
            scaled[quarter, group] = (product.reshape(owners, rows, cw) * weight).astype(
                jnp.bfloat16)

    pair_far = remote(scaled.at[across], pair_in.at[1], ps_.at[1], pr_.at[1], {"tp": near})
    pair_own = remote(scaled.at[near], pair_in.at[0], ps_.at[0], pr_.at[0], {"tp": near})
    down(across)
    pair_far.start()
    down(far)
    down(near)
    pair_own.start()

    def half_out(step):
        p = peer(step)
        return remote(half.at[p], half_in.at[p], us_.at[step], ur_.at[step], {"tp": far})

    def share_out(step):
        return remote(share.at[peer(step)], share_in.at[e], vs_.at[step], vr_.at[step],
                      {"ep": peer(step)})

    def share_land(step):
        return remote(share.at[peer(step)], share_in.at[source(step)], vs_.at[step],
                      vr_.at[step], {"ep": peer(step)})

    pair_far.wait_recv()

    def send_half(step):
        p = peer(step)
        half[p] = (scaled[far, p].astype(jnp.float32) + pair_in[1, p].astype(jnp.float32)).astype(
            jnp.bfloat16)
        half_out(step).start()

    pl.loop(1, ep_count)(send_half)
    send_half(0)
    down(t)
    pair_own.wait_recv()

    def reduced(step):
        p = peer(step)
        half_out(step).wait_recv()
        return (scaled[t, p].astype(jnp.float32) + pair_in[0, p].astype(jnp.float32)
                + half_in[p].astype(jnp.float32)).astype(jnp.bfloat16)

    @pl.loop(1, ep_count)
    def _(step):
        share[peer(step)] = reduced(step)
        share_out(step).start()

    share_in[e] = reduced(0)

    @pl.loop(1, ep_count)
    def _(step):
        share_land(step).wait_recv()

    routed = jnp.sum(share_in[...].astype(jnp.float32), axis=0)
    out_ref[...] = (held[e, t].astype(jnp.float32) + routed).astype(jnp.bfloat16)

    for step in range(1, tp_count):
        attn_out(step).wait_send()
    pair_far.wait_send()
    pair_own.wait_send()

    @pl.loop(1, ep_count)
    def _(step):
        table_out(step).wait_send()
        row_out(step).wait_send()
        share_out(step).wait_send()

    @pl.loop(0, ep_count)
    def _(step):
        far_out(step).wait_send()
        near_out(step).wait_send()
        relay_out(step).wait_send()
        half_out(step).wait_send()


def run_experts(cell, tokens, gain, table, w_proj, w_gate, w_up, w_down):
    ep_count = lax.axis_size("ep")
    tp_count = lax.axis_size("tp")
    rows, width = tokens.shape
    cw = width // tp_count
    hidden = w_gate.shape[2]
    bf16 = jnp.bfloat16
    vmem = pl.BlockSpec(memory_space=pltpu.VMEM)
    hbm = pl.BlockSpec(memory_space=pl.ANY)
    dma = pltpu.SemaphoreType.DMA
    block = (ep_count, rows, cw)
    return pl.pallas_call(
        functools.partial(experts_kernel, ep_count, tp_count),
        out_shape=jax.ShapeDtypeStruct((rows, cw), bf16),
        in_specs=[vmem] * 5 + [hbm] * 3,
        out_specs=vmem,
        scratch_shapes=[
            pltpu.VMEM((width, hidden), bf16),
            pltpu.VMEM((width, hidden), bf16),
            pltpu.VMEM((hidden, width), bf16),
            pltpu.VMEM((tp_count, rows, cw), bf16),
            pltpu.VMEM((tp_count, rows, cw), bf16),
            pltpu.VMEM((ep_count, tp_count, rows, cw), bf16),
            pltpu.VMEM((ep_count * rows, width), bf16),
            pltpu.VMEM((ep_count * rows, hidden), bf16),
            pltpu.VMEM((ep_count,) + table.shape, jnp.float32),
            pltpu.VMEM((tp_count,) + block, bf16),
            pltpu.VMEM((2,) + block, bf16),
            pltpu.VMEM(block, bf16),
            pltpu.VMEM(block, bf16),
            pltpu.VMEM(block, bf16),
            pltpu.VMEM(block, bf16),
            dma((3,)),
            dma((tp_count,)), dma((tp_count,)),
        ] + [dma((ep_count,)) for _ in range(12 - 2)] + [dma((2,)), dma((2,))] + [
            dma((ep_count,)) for _ in range(4)],
        compiler_params=pltpu.CompilerParams(
            collective_id=1, has_side_effects=True, vmem_limit_bytes=60 << 20),
        name="run_experts",
    )(cell, tokens, gain.reshape(1, -1), table, w_proj, w_gate, w_up, w_down)


def body(
    tokens,
    gain_mix,
    gain_ffn,
    w_query,
    w_key,
    w_value,
    w_outgate,
    w_ingate,
    w_forget,
    bias_in,
    bias_forget,
    w_proj,
    matrix_state,
    normal_state,
    stab_state,
    route_ids,
    route_weights,
    w_exp_gate,
    w_exp_up,
    w_exp_down,
):
    ep_count = lax.axis_size("ep")
    tp_index = lax.axis_index("tp")
    seq_dev = tokens.shape[0]
    heads_dev = matrix_state.shape[1]
    head_dim = matrix_state.shape[2]
    head_cols = w_query.shape[1]
    experts = ep_count // 2
    normed = rms_scale(tokens, gain_mix)
    projected = gather_project(tokens, gain_mix, (w_query, w_key, w_value, w_outgate))
    query, key_rows, value_rows, gate_rows = [
        projected[index].reshape(seq_dev, heads_dev, head_dim) for index in range(4)
    ]
    head_first = tp_index * heads_dev
    in_pre = lax.dynamic_slice_in_dim(
        jnp.dot(normed, w_ingate, preferred_element_type=jnp.float32) + bias_in,
        head_first,
        heads_dev,
        1,
    )
    forget_pre = lax.dynamic_slice_in_dim(
        jnp.dot(normed, w_forget, preferred_element_type=jnp.float32) + bias_forget,
        head_first,
        heads_dev,
        1,
    )
    hidden, matrix_new, normal_new, stab_new = memory_step(
        query,
        key_rows,
        value_rows,
        gate_rows,
        in_pre,
        forget_pre,
        matrix_state,
        normal_state,
        stab_state,
    )
    cell = hidden.reshape(seq_dev, head_cols).astype(jnp.bfloat16)
    weights = route_weights / jnp.sum(route_weights, axis=-1, keepdims=True)
    lanes = -(-experts // 128) * 128
    named = route_ids[:, :, None] == jnp.arange(lanes, dtype=jnp.int32)[None, None, :]
    table = jnp.sum(jnp.where(named, weights[:, :, None], 0.0), axis=1)
    mixed_out = run_experts(
        cell, tokens, gain_ffn, table, w_proj, w_exp_gate, w_exp_up, w_exp_down
    )
    return (mixed_out, matrix_new, normal_new, stab_new)


def solution(mesh):
    placed = (
        P("ep", None),
        P(),
        P(),
        P("ep", "tp"),
        P("ep", "tp"),
        P("ep", "tp"),
        P("ep", "tp"),
        P(),
        P(),
        P(),
        P(),
        P("tp", None),
        P("ep", "tp", None, None),
        P("ep", "tp", None),
        P("ep", "tp"),
        P("ep", None),
        P("ep", None),
        P("ep", None, "tp"),
        P("ep", None, "tp"),
        P("ep", "tp", None),
    )
    return jax.shard_map(
        body,
        mesh=mesh,
        in_specs=placed,
        out_specs=(P("ep", "tp"), P("ep", "tp", None, None), P("ep", "tp", None), P("ep", "tp")),
        check_vma=False,
    )
```
